32 devices in a mesh: grp: 2 (over y), fs: 4 (over z), tp: 4 (over x, core).
Axes of the slice: x: 2, y: 2, z: 4, core: 2. Of those that a mesh axis runs over, the one named last changes fastest.
Arguments:
- tokens: bfloat16 [1024, 2048], P(('grp', 'fs')), parts along dimension 0, may hold values from -12 to 12, as said below
- mix_heads: bfloat16 [1024, 2048], P(('grp', 'fs'), 'tp'), parts along dimension 0, may hold values from -6 to 6
- norm_first: float32 [2048], replicated, may hold values from 0.1 to 1.9
- gate_first: bfloat16 [2048, 5632], P('fs', 'tp'), may hold values from -0.125 to 0.125
- up_first: bfloat16 [2048, 5632], P('fs', 'tp'), may hold values from -0.125 to 0.125
- down_first: bfloat16 [5632, 2048], P('tp', 'fs'), may hold values from -0.078125 to 0.078125
- out_weight: bfloat16 [2048, 2048], P('tp', 'fs'), may hold values from -0.125 to 0.125
- norm_second: float32 [2048], replicated, may hold values from 0.1 to 1.9
- gate_second: bfloat16 [2048, 5632], P('fs', 'tp'), may hold values from -0.125 to 0.125
- up_second: bfloat16 [2048, 5632], P('fs', 'tp'), may hold values from -0.125 to 0.125
- down_second: bfloat16 [5632, 2048], P('tp', 'fs'), may hold values from -0.078125 to 0.078125
Outputs:
- layer_out: bfloat16 [1024, 2048], P(('grp', 'fs')), parts along dimension 0
The draws below stay inside these ranges and needn't reach their ends.
There are 2 independent parts, one for each index of `grp`. The reference program is written for one: setup_inputs(seed, part) draws one part's arguments, and reference() takes and returns one part's arrays. A program takes and returns all parts, laid end to end along the dimension named above; an argument that names none is the same for every part. Nothing has to cross between parts.
Inputs may be any that keep to these rules, and one draw needn't show every extreme that they name: Each row of tokens carries a scale of its own.
All inputs are finite; a program needn't handle non-finite values.
Results may differ from the reference program's by a relative error of at most 0.014.
Values may be sent and summed in bfloat16 or wider, within the bound.
No kernel may reach another device: no remote copies, remote signals or barrier semaphores. Data moves between devices by JAX's collectives and lax.ppermute only.
A program may use at most 64 MiB of HBM per device.

```python
import math
import jax
import jax.numpy as jnp
from jax import lax

D = 2048
FF = 5632
MIX = 2048
TOKENS = 512
N_TP = 4


def draw_tokens(key, part):
    subkeys = jax.random.split(key, 3)
    base_values = jax.random.normal(subkeys[0], (TOKENS, D), jnp.float32)
    row_scale = jnp.exp(jax.random.uniform(subkeys[1], (TOKENS, 1), jnp.float32, math.log(0.4), math.log(2.5)))
    values = base_values * row_scale
    return jnp.clip(values, -12.0, 12.0).astype(jnp.bfloat16)


def levels(key, dims, cuts, smallest, largest):
    loudness, own = 1.0, jax.random.fold_in(key, 6)
    for position, shards_of in cuts:
        steps = jnp.exp(jax.random.uniform(jax.random.fold_in(own, position), (shards_of,), jnp.float32, smallest / len(cuts), largest / len(cuts)))
        loudness = loudness * jnp.repeat(steps, dims[position] // shards_of).reshape([-1 if axis == position else 1 for axis in range(len(dims))])
    return loudness


def centred(stream_key, dims, deviation, most, cuts=(), dtype=jnp.bfloat16):
    level = levels(stream_key, dims, cuts, -0.22, 0.18) if cuts else 1.0
    entries = jax.random.normal(stream_key, dims, jnp.float32) * deviation * level
    return jnp.minimum(jnp.maximum(entries, -most), most).astype(dtype)


def setup_inputs(seed: int = 0, part: int = 0) -> dict:
    keys = jax.random.split(jax.random.key(seed), 12)
    part_keys = jax.random.split(jax.random.fold_in(keys[11], part), 12)
    return {
        "tokens": draw_tokens(jax.random.fold_in(jax.random.fold_in(keys[11], part), 71), part),
        "mix_heads": centred(part_keys[1], (TOKENS, MIX), 1.0, 6.0, ((0, 4), (1, 4))),
        "norm_first": jnp.clip(1.0 + 0.18 * jax.random.normal(keys[2], (D,), jnp.float32), 0.1, 1.9),
        "gate_first": centred(keys[3], (D, FF), D ** -0.5, 0.125, ((0, 4), (1, 4))),
        "up_first": centred(keys[4], (D, FF), D ** -0.5, 0.125, ((0, 4), (1, 4))),
        "down_first": centred(keys[5], (FF, D), FF ** -0.5, 0.078125, ((0, 4), (1, 4))),
        "out_weight": centred(keys[6], (MIX, D), MIX ** -0.5, 0.125, ((0, 4), (1, 4))),
        "norm_second": jnp.clip(1.0 + 0.18 * jax.random.normal(keys[7], (D,), jnp.float32), 0.1, 1.9),
        "gate_second": centred(keys[8], (D, FF), D ** -0.5, 0.125, ((0, 4), (1, 4))),
        "up_second": centred(keys[9], (D, FF), D ** -0.5, 0.125, ((0, 4), (1, 4))),
        "down_second": centred(keys[10], (FF, D), FF ** -0.5, 0.078125, ((0, 4), (1, 4))),
    }


EPS = 0.1

def norm_rows(row_block, gain_vector):
    widened = row_block.astype(jnp.float32)
    scaled = widened * lax.rsqrt(lax.optimization_barrier(jnp.mean(widened * widened, axis=-1, keepdims=True)) + EPS)
    return (scaled * gain_vector.astype(jnp.float32)).astype(jnp.bfloat16)

def branch_terms(normed, gate_weight, value_weight, down_weight, added_term):
    block_width = FF // N_TP

    def block_term(index):
        first_col = (index * block_width).astype(jnp.int32)
        gates = jnp.dot(normed, lax.dynamic_slice_in_dim(gate_weight, first_col, block_width, 1), preferred_element_type=jnp.float32)
        values = jnp.dot(normed, lax.dynamic_slice_in_dim(value_weight, first_col, block_width, 1), preferred_element_type=jnp.float32)
        hidden = (jax.nn.silu(gates) * values).astype(jnp.bfloat16)
        partial_value = 0.5 * jnp.dot(hidden, lax.dynamic_slice_in_dim(down_weight, first_col, block_width, 0), preferred_element_type=jnp.float32)
        return partial_value + added_term(index)

    def accumulate(index, total):
        rounded = lax.optimization_barrier(block_term(index).astype(jnp.bfloat16))
        return total + rounded.astype(jnp.float32)
    start_total = jnp.zeros((normed.shape[0], down_weight.shape[1]), jnp.float32)
    return lax.fori_loop(0, N_TP, accumulate, start_total)

def reference(tokens, mix_heads, norm_first, gate_first, up_first, down_first, out_weight, norm_second, gate_second, up_second, down_second):
    head_width = MIX // N_TP

    def head_term(index):
        first_col = (index * head_width).astype(jnp.int32)
        heads = lax.dynamic_slice_in_dim(mix_heads, first_col, head_width, 1)
        weight_rows = lax.dynamic_slice_in_dim(out_weight, first_col, head_width, 0)
        return jnp.dot(heads, weight_rows, preferred_element_type=jnp.float32)

    def no_term(index):
        return jnp.zeros((tokens.shape[0], tokens.shape[1]), jnp.float32)
    normed_one = norm_rows(tokens, norm_first)
    mixed_sum = branch_terms(normed_one, gate_first, up_first, down_first, head_term)
    resid_two = tokens.astype(jnp.float32) + mixed_sum
    normed_two = norm_rows(resid_two, norm_second)
    ffn_sum = branch_terms(normed_two, gate_second, up_second, down_second, no_term)
    return (resid_two + ffn_sum).astype(jnp.bfloat16)
```

```python
import jax
import jax.numpy as jnp
from jax import lax
from jax.sharding import PartitionSpec as P

EPS = 0.1


def shift_exchange(pieces, axis):
    n = len(pieces)
    return [pieces[0]] + [
        lax.ppermute(pieces[s], axis, [(i, (i - s) % n) for i in range(n)]) for s in range(1, n)
    ]


def line_sum(partial_of, n, axis):
    from_left = from_right = None
    for step in range(1, n):
        to_right = partial_of(step)
        to_left = partial_of(n - step)
        if step > 1:
            to_right = to_right + from_left.astype(jnp.float32)
            to_left = to_left + from_right.astype(jnp.float32)
        from_left = lax.ppermute(
            to_right.astype(jnp.bfloat16), axis, [(i, i + 1) for i in range(step)]
        )
        from_right = lax.ppermute(
            to_left.astype(jnp.bfloat16), axis, [(i, i - 1) for i in range(n - step, n)]
        )
    total = partial_of(0)
    if n > 1:
        total = total + from_left.astype(jnp.float32) + from_right.astype(jnp.float32)
    return total


def line_gather(block, n, axis):
    rightward, leftward = [block], [block]
    for step in range(1, n):
        rightward.append(lax.ppermute(rightward[-1], axis, [(i, i + 1) for i in range(step - 1, n - 1)]))
        leftward.append(lax.ppermute(leftward[-1], axis, [(i, i - 1) for i in range(1, n - step + 1)]))
    index = lax.axis_index(axis)
    return [block] + [
        jnp.where(index >= s, rightward[s], leftward[n - s]) for s in range(1, n)
    ]


def dot(left, right):
    return jnp.dot(left, right, preferred_element_type=jnp.float32)


def hidden_of(operands, gate_weight, value_weight, scale, n):
    gates = line_sum(lambda s: dot(operands[s], gate_weight), n, "fs")
    values = line_sum(lambda s: dot(operands[s], value_weight), n, "fs")
    return (jax.nn.silu(gates * scale) * (values * scale)).astype(jnp.bfloat16)


def share_sum(terms, nt):
    stacked = jnp.stack(terms)
    n, rows, cols = stacked.shape
    by_share = stacked.reshape(n, nt, rows // nt, cols)
    index = lax.axis_index("tp")
    pieces = [
        lax.dynamic_index_in_dim(by_share, (index - s) % nt, 1, keepdims=False) for s in range(nt)
    ]
    got = shift_exchange(pieces, "tp")
    total = got[0].astype(jnp.float32)
    for piece in got[1:]:
        total = total + piece.astype(jnp.float32)
    return total


def from_relative(stacked, index):
    n = stacked.shape[0]
    return lax.dynamic_slice_in_dim(jnp.concatenate([stacked, stacked]), (n - index) % n, n, 0)


def local(
    tokens,
    mix_heads,
    norm_first,
    gate_first,
    up_first,
    down_first,
    out_weight,
    norm_second,
    gate_second,
    up_second,
    down_second,
):
    n, nt = lax.axis_size("fs"), lax.axis_size("tp")
    i, j = lax.axis_index("fs"), lax.axis_index("tp")
    rows, width = tokens.shape
    cols = width // n
    share = rows // nt
    gain_one = lax.dynamic_slice_in_dim(norm_first, i * cols, cols)
    gain_two = lax.dynamic_slice_in_dim(norm_second, i * cols, cols)

    widened = tokens.astype(jnp.float32)
    scale_one = lax.rsqrt(jnp.mean(widened * widened, axis=-1, keepdims=True) + EPS)
    pieces = [
        lax.dynamic_slice_in_dim(tokens, ((i + s) % n) * cols, cols, 1) for s in range(n)
    ]
    own_cols = [pieces[0]] + [
        lax.ppermute(pieces[s], "fs", [(a, (a + s) % n) for a in range(n)]) for s in range(1, n)
    ]
    operands = [(x.astype(jnp.float32) * gain_one).astype(jnp.bfloat16) for x in own_cols]
    heads = line_gather(mix_heads, n, "fs")
    hidden = line_gather(hidden_of(operands, gate_first, up_first, scale_one, n), n, "fs")
    terms = [
        (0.5 * dot(hidden[s], down_first) + dot(heads[s], out_weight)).astype(jnp.bfloat16)
        for s in range(n)
    ]
    mixed = share_sum(terms, nt)
    own_rows = jnp.stack([lax.dynamic_slice_in_dim(x, j * share, share, 0) for x in own_cols])
    resid_two = own_rows.astype(jnp.float32) + mixed

    squares = jnp.sum(resid_two * resid_two, axis=-1)
    gathered = lax.all_gather((resid_two * gain_two).astype(jnp.bfloat16), "tp", axis=0)
    operands = [gathered[:, s].reshape(rows, cols) for s in range(n)]
    got = [squares[0]] + [
        lax.ppermute(squares[s], "fs", [(a, (a - s) % n) for a in range(n)]) for s in range(1, n)
    ]
    own_squares = lax.all_gather(sum(got[1:], got[0]), "tp", axis=0, tiled=True)
    scale_two = lax.rsqrt(own_squares[:, None] / width + EPS)
    hidden = line_gather(hidden_of(operands, gate_second, up_second, scale_two, n), n, "fs")
    terms = [(0.5 * dot(hidden[s], down_second)).astype(jnp.bfloat16) for s in range(n)]
    finished = (resid_two + share_sum(terms, nt)).astype(jnp.bfloat16)
    got = jnp.stack(shift_exchange([finished[s] for s in range(n)], "fs"))
    whole = jnp.moveaxis(from_relative(got, i), 0, 1).reshape(share, width)
    return lax.all_gather(whole, "tp", axis=0, tiled=True)


def solution(mesh):
    in_specs = (
        P(("grp", "fs"), None),
        P(("grp", "fs"), "tp"),
        P(),
        P("fs", "tp"),
        P("fs", "tp"),
        P("tp", "fs"),
        P("tp", "fs"),
        P(),
        P("fs", "tp"),
        P("fs", "tp"),
        P("tp", "fs"),
    )
    out_specs = P(("grp", "fs"), None)
    return jax.shard_map(local, mesh=mesh, in_specs=in_specs, out_specs=out_specs, check_vma=False)
```

```python
import jax
import jax.numpy as jnp
from jax import lax
from jax.sharding import PartitionSpec as P

EPS = 0.1


def shift_exchange(pieces, axis):
    n = len(pieces)
    return [pieces[0]] + [
        lax.ppermute(pieces[s], axis, [(i, (i - s) % n) for i in range(n)]) for s in range(1, n)
    ]


def line_gather(block, n, axis):
    rightward, leftward = [block], [block]
    for step in range(1, n):
        rightward.append(lax.ppermute(rightward[-1], axis, [(i, i + 1) for i in range(step - 1, n - 1)]))
        leftward.append(lax.ppermute(leftward[-1], axis, [(i, i - 1) for i in range(1, n - step + 1)]))
    index = lax.axis_index(axis)
    return [block] + [
        jnp.where(index >= s, rightward[s], leftward[n - s]) for s in range(1, n)
    ]


def dot(left, right):
    return jnp.dot(left, right, preferred_element_type=jnp.float32)


def norm_rows(row_block, gain_vector):
    widened = row_block.astype(jnp.float32)
    scaled = widened * lax.rsqrt(jnp.mean(widened * widened, axis=-1, keepdims=True) + EPS)
    return (scaled * gain_vector).astype(jnp.bfloat16)


def unit_slices(gate_weight, value_weight):
    n, ng = lax.axis_size("fs"), lax.axis_size("grp")
    i, g = lax.axis_index("fs"), lax.axis_index("grp")
    rows, units = gate_weight.shape
    part, width = rows // ng, units // n

    def cut(first_row, height, s):
        corner = (first_row, ((i + s) % n) * width)
        return jnp.stack(
            [lax.dynamic_slice(w, corner, (height, width)) for w in (gate_weight, value_weight)]
        )

    blocks = [cut(0, rows, 0)]
    for s in range(1, n):
        fetched = lax.ppermute(cut(g * part, part, s), "fs", [(a, (a + s) % n) for a in range(n)])
        parts = shift_exchange([fetched] * ng, "grp")
        ordered = from_relative(jnp.stack(parts), g)
        blocks.append(jnp.moveaxis(ordered, 0, 1).reshape(2, rows, width))
    return blocks


def hidden_slice(column_blocks, weights):
    gates = sum(dot(x, w[0]) for x, w in zip(column_blocks, weights))
    values = sum(dot(x, w[1]) for x, w in zip(column_blocks, weights))
    return (jax.nn.silu(gates) * values).astype(jnp.bfloat16)


def down_terms(hidden, down_weight):
    n, i = lax.axis_size("fs"), lax.axis_index("fs")
    width = down_weight.shape[0] // n
    return 0.5 * sum(
        dot(h, lax.dynamic_slice_in_dim(down_weight, ((i - s) % n) * width, width, 0))
        for s, h in enumerate(hidden)
    )


def share_gather(block, nt):
    per = 2 if nt % 2 == 0 else 1
    lines = nt // per
    mine = [block]
    for s in range(1, lines):
        mine.append(
            lax.ppermute(block, "tp", [(a, (a + per * s) % nt) for a in range(nt)])
        )
    if per == 1:
        return mine
    swapped = [lax.ppermute(b, "tp", [(a, a ^ 1) for a in range(nt)]) for b in mine]
    odd = lax.axis_index("tp") % 2 == 1
    result = []
    for s in range(lines):
        result.append(mine[s])
        result.append(jnp.where(odd, swapped[s], swapped[(s + 1) % lines]))
    return result


def share_sum(terms, nt):
    pieces = terms.reshape(nt, terms.shape[0] // nt, terms.shape[1])
    got = shift_exchange([pieces[s] for s in range(nt)], "tp")
    total = got[0].astype(jnp.float32)
    for piece in got[1:]:
        total = total + piece.astype(jnp.float32)
    return total


def from_relative(stacked, index):
    n = stacked.shape[0]
    return lax.dynamic_slice_in_dim(jnp.concatenate([stacked, stacked]), (n - index) % n, n, 0)


def from_descending(blocks, index):
    n = len(blocks)
    backward = jnp.stack([blocks[0]] + blocks[:0:-1])
    return from_relative(backward, index)


def local(
    tokens,
    mix_heads,
    norm_first,
    gate_first,
    up_first,
    down_first,
    out_weight,
    norm_second,
    gate_second,
    up_second,
    down_second,
):
    n, nt = lax.axis_size("fs"), lax.axis_size("tp")
    i, j = lax.axis_index("fs"), lax.axis_index("tp")
    rows, width = tokens.shape
    cols = width // n
    share = rows // nt

    own = norm_rows(lax.dynamic_slice_in_dim(tokens, j * share, share, 0), norm_first)
    column = from_descending(line_gather(own, n, "fs"), i).reshape(n * share, width)
    normed = jnp.concatenate(share_gather(column, nt))
    own_tokens = lax.dynamic_slice_in_dim(tokens, j * share, share, 0)
    pieces = [
        lax.dynamic_slice_in_dim(own_tokens, ((i + s) % n) * cols, cols, 1) for s in range(n)
    ]
    own_cols = [pieces[0]] + [
        lax.ppermute(pieces[s], "fs", [(a, (a + s) % n) for a in range(n)]) for s in range(1, n)
    ]
    own_cols = from_descending(own_cols, i).reshape(n * share, cols)
    weights_one = unit_slices(gate_first, up_first)
    blocks = [
        lax.dynamic_slice_in_dim(normed, ((i - s) % n) * cols, cols, 1) for s in range(n)
    ]
    hidden = line_gather(hidden_slice(blocks, weights_one), n, "fs")
    heads = from_descending(line_gather(mix_heads, n, "fs"), i)
    heads = heads.reshape(n, nt, share, heads.shape[-1])
    heads = jnp.stack(
        [lax.dynamic_index_in_dim(heads, (j - s) % nt, 1, keepdims=False) for s in range(nt)]
    ).reshape(n * rows, heads.shape[-1])
    terms = down_terms(hidden, down_first) + dot(heads, out_weight)
    resid_two = own_cols.astype(jnp.float32) + share_sum(terms.astype(jnp.bfloat16), nt)

    weights_two = unit_slices(gate_second, up_second)
    by_column = jnp.stack(line_gather(resid_two.astype(jnp.bfloat16), n, "fs"))
    gathered = jnp.concatenate(share_gather(by_column, nt), axis=1).astype(jnp.float32)
    scale = lax.rsqrt(jnp.sum(gathered * gathered, axis=(0, 2))[:, None] / width + EPS)
    blocks = [
        (
            gathered[s] * scale * lax.dynamic_slice_in_dim(norm_second, ((i - s) % n) * cols, cols)
        ).astype(jnp.bfloat16)
        for s in range(n)
    ]
    hidden = line_gather(hidden_slice(blocks, weights_two), n, "fs")
    terms = down_terms(hidden, down_second)
    finished = resid_two + share_sum(terms.astype(jnp.bfloat16), nt)
    finished = finished.astype(jnp.bfloat16).reshape(n, share, cols)
    pieces = [
        lax.dynamic_index_in_dim(finished, (i - s) % n, 0, keepdims=False) for s in range(n)
    ]
    got = jnp.stack(shift_exchange(pieces, "fs"))
    whole = jnp.moveaxis(from_relative(got, i), 0, 1).reshape(share, width)
    return lax.all_gather(whole, "tp", axis=0, tiled=True)


def solution(mesh):
    in_specs = (
        P(("grp", "fs"), None),
        P(("grp", "fs"), "tp"),
        P(),
        P("fs", "tp"),
        P("fs", "tp"),
        P("tp", "fs"),
        P("tp", "fs"),
        P(),
        P("fs", "tp"),
        P("fs", "tp"),
        P("tp", "fs"),
    )
    out_specs = P(("grp", "fs"), None)
    return jax.shard_map(local, mesh=mesh, in_specs=in_specs, out_specs=out_specs, check_vma=False)
```

```python
import jax
import jax.numpy as jnp
from jax import lax
from jax.sharding import PartitionSpec as P

EPS = 0.1


def shift_exchange(pieces, axis):
    n = len(pieces)
    return [pieces[0]] + [
        lax.ppermute(pieces[s], axis, [(i, (i - s) % n) for i in range(n)]) for s in range(1, n)
    ]


def line_sum(partial_of, n, axis):
    from_left = from_right = None
    for step in range(1, n):
        to_right = partial_of(step)
        to_left = partial_of(n - step)
        if step > 1:
            to_right = to_right + from_left.astype(jnp.float32)
            to_left = to_left + from_right.astype(jnp.float32)
        from_left = lax.ppermute(
            to_right.astype(jnp.bfloat16), axis, [(i, i + 1) for i in range(step)]
        )
        from_right = lax.ppermute(
            to_left.astype(jnp.bfloat16), axis, [(i, i - 1) for i in range(n - step, n)]
        )
    total = partial_of(0)
    if n > 1:
        total = total + from_left.astype(jnp.float32) + from_right.astype(jnp.float32)
    return total


def line_gather(block, n, axis):
    rightward, leftward = [block], [block]
    for step in range(1, n):
        rightward.append(lax.ppermute(rightward[-1], axis, [(i, i + 1) for i in range(step - 1, n - 1)]))
        leftward.append(lax.ppermute(leftward[-1], axis, [(i, i - 1) for i in range(1, n - step + 1)]))
    index = lax.axis_index(axis)
    return [block] + [
        jnp.where(index >= s, rightward[s], leftward[n - s]) for s in range(1, n)
    ]


def dot(left, right):
    return jnp.dot(left, right, preferred_element_type=jnp.float32)


def hidden_of(operands, gate_weight, value_weight, scale, n):
    gates = line_sum(lambda s: dot(operands[s], gate_weight), n, "fs")
    values = line_sum(lambda s: dot(operands[s], value_weight), n, "fs")
    return (jax.nn.silu(gates * scale) * (values * scale)).astype(jnp.bfloat16)


def share_sum(terms, nt):
    stacked = jnp.stack(terms)
    n, rows, cols = stacked.shape
    by_share = stacked.reshape(n, nt, rows // nt, cols)
    index = lax.axis_index("tp")
    pieces = [
        lax.dynamic_index_in_dim(by_share, (index - s) % nt, 1, keepdims=False) for s in range(nt)
    ]
    got = shift_exchange(pieces, "tp")
    total = got[0].astype(jnp.float32)
    for piece in got[1:]:
        total = total + piece.astype(jnp.float32)
    return total


def from_relative(stacked, index):
    n = stacked.shape[0]
    return lax.dynamic_slice_in_dim(jnp.concatenate([stacked, stacked]), (n - index) % n, n, 0)


def local(
    tokens,
    mix_heads,
    norm_first,
    gate_first,
    up_first,
    down_first,
    out_weight,
    norm_second,
    gate_second,
    up_second,
    down_second,
):
    n, nt = lax.axis_size("fs"), lax.axis_size("tp")
    i, j = lax.axis_index("fs"), lax.axis_index("tp")
    rows, width = tokens.shape
    cols = width // n
    share = rows // nt
    gain_one = lax.dynamic_slice_in_dim(norm_first, i * cols, cols)
    gain_two = lax.dynamic_slice_in_dim(norm_second, i * cols, cols)

    widened = tokens.astype(jnp.float32)
    scale_one = lax.rsqrt(jnp.mean(widened * widened, axis=-1, keepdims=True) + EPS)
    pieces = [
        lax.dynamic_slice_in_dim(tokens, ((i + s) % n) * cols, cols, 1) for s in range(n)
    ]
    own_cols = [pieces[0]] + [
        lax.ppermute(pieces[s], "fs", [(a, (a + s) % n) for a in range(n)]) for s in range(1, n)
    ]
    operands = [(x.astype(jnp.float32) * gain_one).astype(jnp.bfloat16) for x in own_cols]
    mix_heads, *operands = lax.optimization_barrier((mix_heads, *operands))
    heads = line_gather(mix_heads, n, "fs")
    hidden = line_gather(hidden_of(operands, gate_first, up_first, scale_one, n), n, "fs")
    terms = [
        (0.5 * dot(hidden[s], down_first) + dot(heads[s], out_weight)).astype(jnp.bfloat16)
        for s in range(n)
    ]
    mixed = share_sum(terms, nt)
    own_rows = jnp.stack([lax.dynamic_slice_in_dim(x, j * share, share, 0) for x in own_cols])
    resid_two = own_rows.astype(jnp.float32) + mixed

    squares = jnp.sum(resid_two * resid_two, axis=-1)
    gathered = lax.all_gather((resid_two * gain_two).astype(jnp.bfloat16), "tp", axis=0)
    operands = [gathered[:, s].reshape(rows, cols) for s in range(n)]
    got = [squares[0]] + [
        lax.ppermute(squares[s], "fs", [(a, (a - s) % n) for a in range(n)]) for s in range(1, n)
    ]
    own_squares = lax.all_gather(sum(got[1:], got[0]), "tp", axis=0, tiled=True)
    scale_two = lax.rsqrt(own_squares[:, None] / width + EPS)
    hidden = line_gather(hidden_of(operands, gate_second, up_second, scale_two, n), n, "fs")
    terms = [(0.5 * dot(hidden[s], down_second)).astype(jnp.bfloat16) for s in range(n)]
    finished = (resid_two + share_sum(terms, nt)).astype(jnp.bfloat16)
    got = jnp.stack(shift_exchange([finished[s] for s in range(n)], "fs"))
    whole = jnp.moveaxis(from_relative(got, i), 0, 1).reshape(share, width)
    return lax.all_gather(whole, "tp", axis=0, tiled=True)


def solution(mesh):
    in_specs = (
        P(("grp", "fs"), None),
        P(("grp", "fs"), "tp"),
        P(),
        P("fs", "tp"),
        P("fs", "tp"),
        P("tp", "fs"),
        P("tp", "fs"),
        P(),
        P("fs", "tp"),
        P("fs", "tp"),
        P("tp", "fs"),
    )
    out_specs = P(("grp", "fs"), None)
    return jax.shard_map(local, mesh=mesh, in_specs=in_specs, out_specs=out_specs, check_vma=False)
```
